32 devices in a mesh: sp: 4 (over z), fs: 4 (over y, x), tp: 2 (over core).
Axes of the slice: x: 2, y: 2, z: 4, core: 2. Of those that a mesh axis runs over, the one named last changes fastest.
Arguments:
- tokens: bfloat16 [1024, 2048], P(('sp', 'fs', 'tp')), may hold values from -6 to 6
- norm_gain: float32 [2048], replicated, may hold values from 0.1 to 1.9
- w_query: bfloat16 [2048, 2048], P(None, ('fs', 'tp')), may hold values from -0.9722718 to 0.9722718
- w_key: bfloat16 [2048, 512], P(None, 'fs'), may hold values from -0.77339804 to 0.77339804
- w_value: bfloat16 [2048, 512], P(None, 'fs'), may hold values from -0.125 to 0.125
- w_conv_value: bfloat16 [2048, 1024], P(None, ('fs', 'tp')), may hold values from -0.125 to 0.125
- w_conv_pre: bfloat16 [2048, 1024], P(None, ('fs', 'tp')), may hold values from -0.125 to 0.125
- w_conv_post: bfloat16 [2048, 1024], P(None, ('fs', 'tp')), may hold values from -0.125 to 0.125
- conv_taps: bfloat16 [3, 1024], replicated, may hold values from -3.5 to 3.5
- log_gate_cache: float32 [16, 1024], replicated, may hold values from -65 to 0, as said below
- w_out_conv: bfloat16 [1024, 2048], P(('fs', 'tp')), may hold values from -0.125 to 0.125
- w_out_attn: bfloat16 [2048, 2048], P(('fs', 'tp')), may hold values from -0.375 to 0.375
Outputs:
- mixed: bfloat16 [1024, 2048], P(('sp', 'fs', 'tp'))
The draws below stay inside these ranges and needn't reach their ends.
Inputs may be any that keep to these rules, and one draw needn't show every extreme that they name: `log_gate_cache`: each row is a cumulative sum over positions of log forget gates, none of them positive.
All inputs are finite; a program needn't handle non-finite values.
Results may differ from the reference program's by a relative error of at most 0.014.
The reference program's roundings to bfloat16 on the way count: a program that leaves them out, or rounds other values in their place, can miss the bound.
Values may be sent and summed in bfloat16 or wider, within the bound.
A program may use at most 64 MiB of HBM per device.

```python
import math
import jax
import jax.numpy as jnp
from jax import lax

D = 2048
QUERY_HEAD_COUNT = 16
KV_HEADS = 4
HEAD_DIM = 128
CHANNELS = 1024
KERNEL = 3
TOK_DEV = 256
SEQUENCE_LENGTH = 1024
N_FS = 4
N_TP = 2


def draw_w_query(key, part):
    entries = jnp.clip(jax.random.normal(jax.random.fold_in(key, 11), (D, QUERY_HEAD_COUNT * HEAD_DIM), jnp.float32), -6.0, 6.0) * (2.5 * D ** (-0.5))
    return entries.astype(jnp.bfloat16)


def draw_w_key(key, part):
    entries = jnp.clip(jax.random.normal(jax.random.fold_in(key, 13), (D, KV_HEADS * HEAD_DIM), jnp.float32), -6.0, 6.0) * D ** (-0.5)
    return entries.astype(jnp.bfloat16)


def draw_log_gate_cache(key, part):
    random_subseeds = jax.random.split(jax.random.fold_in(key, 23), 5)
    head_order = jax.random.permutation(random_subseeds[0], QUERY_HEAD_COUNT)
    fast_count = QUERY_HEAD_COUNT // 2
    fast_heads = head_order < fast_count
    block_count = SEQUENCE_LENGTH // TOK_DEV
    block_rate = jnp.exp(jax.random.uniform(random_subseeds[1], (QUERY_HEAD_COUNT, block_count), jnp.float32, -math.log(2.0), math.log(2.0)))
    jitter = jax.random.uniform(random_subseeds[2], (QUERY_HEAD_COUNT, SEQUENCE_LENGTH), jnp.float32, 0.5, 1.5)
    increment_frequency = jnp.repeat(block_rate, TOK_DEV, axis=1) * jitter
    baseline_frequency = jnp.where(fast_heads[:, None], 1.0 / min(50, TOK_DEV), 0.5 / SEQUENCE_LENGTH)
    spike_position = jax.random.randint(random_subseeds[3], (QUERY_HEAD_COUNT, 3), 0, SEQUENCE_LENGTH)
    spike_length = jax.random.uniform(random_subseeds[4], (QUERY_HEAD_COUNT, 3), jnp.float32, math.log(0.5), math.log(0.8))
    sequence_places = jnp.arange(SEQUENCE_LENGTH, dtype=jnp.int32)
    spike_events = jnp.sum(jnp.where(sequence_places[None, None, :] == spike_position[:, :, None], spike_length[:, :, None], 0.0), axis=1)
    return jnp.cumsum(spike_events - baseline_frequency * increment_frequency, axis=1)


def block_levels(own_key, dims, cuts, least, top_value):
    loudness = 1.0
    for dim, shards_of in cuts:
        heights = jax.random.uniform(jax.random.fold_in(jax.random.fold_in(own_key, 6), dim), (shards_of,), jnp.float32, least / len(cuts), top_value / len(cuts))
        loudness = loudness * jnp.repeat(jnp.exp(heights), dims[dim] // shards_of).reshape((-1,) + (1,) * (len(dims) - 1 - dim))
    return loudness


def gaussian(own_key, extent, scale, limit, pieces=(), kind=jnp.bfloat16):
    result = jax.random.normal(own_key, extent, jnp.float32) * scale
    if len(pieces) > 0:
        result = block_levels(own_key, extent, pieces, -0.22, 0.18) * result
    return jnp.clip(result, min=-limit, max=limit).astype(kind)


def setup_inputs(seed: int = 0) -> dict:
    arg_keys = jax.random.split(jax.random.key(seed), 13)
    return {
        "tokens": gaussian(arg_keys[0], (SEQUENCE_LENGTH, D), 1.0, 6.0, ((0, 32),)),
        "norm_gain": jnp.clip(1.0 + 0.18 * jax.random.normal(arg_keys[1], (D,), jnp.float32), 0.1, 1.9),
        "w_query": draw_w_query(jax.random.fold_in(arg_keys[12], 71), 0),
        "w_key": draw_w_key(jax.random.fold_in(arg_keys[12], 71), 0),
        "w_value": gaussian(arg_keys[4], (D, KV_HEADS * HEAD_DIM), D ** -0.5, 0.125, ((1, 4),)),
        "w_conv_value": gaussian(arg_keys[5], (D, CHANNELS), D ** -0.5, 0.125, ((1, 8),)),
        "w_conv_pre": gaussian(arg_keys[6], (D, CHANNELS), D ** -0.5, 0.125, ((1, 8),)),
        "w_conv_post": gaussian(arg_keys[7], (D, CHANNELS), D ** -0.5, 0.125, ((1, 8),)),
        "conv_taps": gaussian(arg_keys[8], (KERNEL, CHANNELS), KERNEL ** -0.5, 3.5),
        "log_gate_cache": draw_log_gate_cache(jax.random.fold_in(arg_keys[12], 71), 0),
        "w_out_conv": gaussian(arg_keys[10], (CHANNELS, D), (2 * CHANNELS) ** -0.5, 0.125, ((0, 8),)),
        "w_out_attn": gaussian(arg_keys[11], (QUERY_HEAD_COUNT * HEAD_DIM, D), (QUERY_HEAD_COUNT * HEAD_DIM // 8) ** -0.5, 0.375, ((0, 8),)),
    }


epsilon = 1e-06
masked_score = -1e+30

def attend_head(inputs):
    queries, keys, values, head_gates = inputs
    span = 512 if SEQUENCE_LENGTH % 512 == 0 else SEQUENCE_LENGTH
    blocks = SEQUENCE_LENGTH // span
    score_scale = HEAD_DIM ** (-0.5)
    query_blocks = queries.reshape(blocks, span, HEAD_DIM)
    gate_blocks = head_gates.reshape(blocks, span)

    def one_block(block_inputs):
        query_rows, gate_rows, block_index = block_inputs
        row_positions = block_index * span + jnp.arange(span, dtype=jnp.int32)

        def absorb(key_index, carry):
            running_max, running_sum, weighted = carry
            key_start = (key_index * span).astype(jnp.int32)
            key_rows = lax.dynamic_slice_in_dim(keys, key_start, span, 0)
            value_rows = lax.dynamic_slice_in_dim(values, key_start, span, 0)
            gate_keys = lax.dynamic_slice_in_dim(head_gates, key_start, span, 0)
            scores = jnp.dot(query_rows, key_rows.T, preferred_element_type=jnp.float32) * score_scale
            scores = scores + gate_rows[:, None] - gate_keys[None, :]
            key_positions = key_start + jnp.arange(span, dtype=jnp.int32)
            scores = jnp.where(row_positions[:, None] >= key_positions[None, :], scores, masked_score)
            new_max = jnp.maximum(running_max, lax.optimization_barrier(jnp.max(scores, axis=1)))
            rescale = jnp.exp(running_max - new_max)
            weights = jnp.exp(scores - new_max[:, None])
            running_sum = running_sum * rescale + lax.optimization_barrier(jnp.sum(weights, axis=1))
            weighted = weighted * rescale[:, None] + jnp.dot(weights.astype(jnp.bfloat16), value_rows, preferred_element_type=jnp.float32)
            return (new_max, running_sum, weighted)
        initial = (jnp.full((span,), masked_score, jnp.float32), jnp.zeros((span,), jnp.float32), jnp.zeros((span, HEAD_DIM), jnp.float32))
        final = lax.fori_loop(0, block_index + 1, absorb, initial)
        return (final[2] / final[1][:, None]).astype(jnp.bfloat16)
    outputs = lax.map(one_block, (query_blocks, gate_blocks, jnp.arange(blocks, dtype=jnp.int32)))
    return outputs.reshape(SEQUENCE_LENGTH, HEAD_DIM)

def reference(tokens, norm_gain, w_query, w_key, w_value, w_conv_value, w_conv_pre, w_conv_post, conv_taps, log_gate_cache, w_out_conv, w_out_attn):
    float_rows = tokens.astype(jnp.float32)
    normed = (float_rows * lax.rsqrt(lax.optimization_barrier(jnp.mean(float_rows * float_rows, axis=1, keepdims=True)) + epsilon) * norm_gain).astype(jnp.bfloat16)

    def project(weight):
        return jnp.dot(normed, weight, preferred_element_type=jnp.float32).astype(jnp.bfloat16)
    post_gate = project(w_conv_post)
    pre_gate = project(w_conv_pre)
    conv_value = project(w_conv_value)
    queries = project(w_query)
    keys = project(w_key)
    values = project(w_value)
    mixed_in = (pre_gate.astype(jnp.float32) * conv_value.astype(jnp.float32)).astype(jnp.bfloat16)
    padded = jnp.concatenate([jnp.zeros((KERNEL - 1, CHANNELS), jnp.bfloat16), mixed_in], axis=0).astype(jnp.float32)
    tap_weights = conv_taps.astype(jnp.float32)
    conv_sum = tap_weights[0] * padded[0:SEQUENCE_LENGTH]
    for offset in range(1, KERNEL):
        conv_sum = conv_sum + tap_weights[offset] * padded[offset:offset + SEQUENCE_LENGTH]
    conv_out = (post_gate.astype(jnp.float32) * conv_sum).astype(jnp.bfloat16)
    query_heads = queries.reshape(SEQUENCE_LENGTH, QUERY_HEAD_COUNT, HEAD_DIM).transpose(1, 0, 2)
    key_heads = jnp.repeat(keys.reshape(SEQUENCE_LENGTH, KV_HEADS, HEAD_DIM).transpose(1, 0, 2), QUERY_HEAD_COUNT // KV_HEADS, axis=0)
    value_heads = jnp.repeat(values.reshape(SEQUENCE_LENGTH, KV_HEADS, HEAD_DIM).transpose(1, 0, 2), QUERY_HEAD_COUNT // KV_HEADS, axis=0)
    attn_heads = lax.map(attend_head, (query_heads, key_heads, value_heads, log_gate_cache))
    attn_out = attn_heads.transpose(1, 0, 2).reshape(SEQUENCE_LENGTH, QUERY_HEAD_COUNT * HEAD_DIM)
    groups = N_FS * N_TP
    conv_width = CHANNELS // groups
    head_width = QUERY_HEAD_COUNT * HEAD_DIM // groups
    mixed = jnp.zeros((SEQUENCE_LENGTH, D), jnp.float32)
    for group in range(groups):
        partial_sum = jnp.dot(conv_out[:, group * conv_width:(group + 1) * conv_width], w_out_conv[group * conv_width:(group + 1) * conv_width], preferred_element_type=jnp.float32)
        partial_sum = partial_sum + jnp.dot(attn_out[:, group * head_width:(group + 1) * head_width], w_out_attn[group * head_width:(group + 1) * head_width], preferred_element_type=jnp.float32)
        mixed = mixed + lax.optimization_barrier(partial_sum.astype(jnp.bfloat16)).astype(jnp.float32)
    return mixed.astype(jnp.bfloat16)
```

```python
import functools

import jax
import jax.numpy as jnp
from jax import lax
from jax.experimental import pallas as pl
from jax.experimental.pallas import tpu as pltpu
from jax.sharding import PartitionSpec as P

epsilon = 1e-06
masked_score = -1e30
MESH = pl.DeviceIdType.MESH
f32 = jnp.float32
bf16 = jnp.bfloat16


def dot(a, b):
    return jnp.dot(a, b, preferred_element_type=f32)


def layer_kernel(
    n_sp,
    n_fs,
    n_tp,
    col_chunk,
    tokens,
    gain,
    w_query,
    w_key,
    w_value,
    w_conv_value,
    w_conv_pre,
    w_conv_post,
    taps,
    gates,
    w_out_conv,
    w_out_attn,
    out,
    normed,
    kv_w,
    pair_w,
    rest_w,
    out_w,
    kv,
    ext,
    tail,
    halo,
    post_buf,
    q_buf,
    gate_col,
    run_max,
    run_sum,
    acc,
    mix_in,
    part,
    sib_in,
    pair_sum,
    rs_in,
    w_sem,
    ag_send,
    ag_recv,
    agf_send,
    agf_recv,
    kv_send,
    kv_recv,
    kvf_send,
    kvf_recv,
    halo_send,
    halo_recv,
    sib_send,
    sib_recv,
    rs_send,
    rs_recv,
):
    s = lax.axis_index("sp")
    f = lax.axis_index("fs")
    t = lax.axis_index("tp")
    g = f * n_tp + t
    own_rows, width = tokens.shape
    block = own_rows * n_fs * n_tp
    channels = w_conv_post.shape[1]
    head_dim = w_key.shape[1]
    heads = w_query.shape[1] // head_dim
    half = block // n_tp
    scale = head_dim ** (-0.5)

    def rc(src, dst, send, recv, device):
        return pltpu.make_async_remote_copy(
            src_ref=src,
            dst_ref=dst,
            send_sem=send,
            recv_sem=recv,
            device_id=device,
            device_id_type=MESH,
        )

    def fs_peer(df):
        return (s, lax.rem(f + df, n_fs), t)

    def tp_peer(dt):
        return (s, f, lax.rem(t + dt, n_tp))

    barrier = pltpu.get_barrier_semaphore()
    for dt in range(1, n_tp):
        pl.semaphore_signal(barrier, inc=1, device_id=tp_peer(dt), device_id_type=MESH)
    for df in range(1, n_fs):
        pl.semaphore_signal(barrier, inc=1, device_id=fs_peer(df), device_id_type=MESH)

    def greet(ds, c):
        pl.semaphore_signal(
            barrier, inc=1, device_id=(lax.rem(s + ds, n_sp), f, t), device_id_type=MESH
        )
        return c

    lax.fori_loop(1, n_sp, greet, 0)

    c0, c1, hd = channels, 2 * channels, head_dim
    qw = w_query.shape[1]
    loads = [
        (w_key, kv_w.at[:, 0:hd]),
        (w_value, kv_w.at[:, hd : 2 * hd]),
        (w_conv_pre, pair_w.at[:, 0:c0]),
        (w_conv_value, pair_w.at[:, c0:c1]),
        (w_query, rest_w.at[:, 0:qw]),
        (w_conv_post, rest_w.at[:, qw : qw + channels]),
        (w_out_conv, out_w.at[0:channels, :]),
        (w_out_attn, out_w.at[channels : channels + qw, :]),
    ]
    load_copies = [
        pltpu.make_async_copy(src, dst, w_sem.at[i]) for i, (src, dst) in enumerate(loads)
    ]
    for cp in load_copies:
        cp.start()

    rows = tokens[...].astype(f32)
    inv = lax.rsqrt(jnp.mean(rows * rows, axis=1, keepdims=True) + epsilon)
    normed[pl.ds(pl.multiple_of(g * own_rows, own_rows), own_rows), :] = (
        rows * inv * gain[...]
    ).astype(bf16)

    pl.semaphore_wait(barrier, (n_tp - 1) + (n_fs - 1) + (n_sp - 1))

    def slot(fi, ti):
        return normed.at[pl.ds(pl.multiple_of((fi * n_tp + ti) * own_rows, own_rows), own_rows), :]

    def ag_copy(df):
        return rc(slot(f, t), slot(f, t), ag_send.at[df], ag_recv.at[df], fs_peer(df))

    def agf_copy(df, dt):
        origin = lax.rem(f - df + n_fs, n_fs)
        i = df * n_tp + dt
        return rc(slot(origin, t), slot(origin, t), agf_send.at[i], agf_recv.at[i], tp_peer(dt))

    for df in range(1, n_fs):
        ag_copy(df).start()
    for dt in range(1, n_tp):
        agf_copy(0, dt).start()

    for h in range(heads):
        row = gates[pl.ds(g * heads + h, 1), pl.ds(pl.multiple_of(s * block, 128), block)]
        gate_col[h] = jnp.broadcast_to(row, (128, block)).T

    for df in range(1, n_fs):
        ag_copy(df).wait_recv()
        for dt in range(1, n_tp):
            agf_copy(df, dt).start()
    for df in range(n_fs):
        for dt in range(1, n_tp):
            agf_copy(df, dt).wait_recv()

    load_copies[0].wait()
    load_copies[1].wait()
    base = pl.multiple_of(s * block, block)
    kv[pl.ds(base, block), :] = dot(normed[...], kv_w[...]).astype(bf16)

    def kv_piece(si, ti):
        return kv.at[pl.ds(pl.multiple_of(si * block + ti * half, half), half), :]

    def kv_copy(ds, origin, dest):
        return rc(
            kv_piece(origin, t), kv_piece(origin, t), kv_send.at[ds], kv_recv.at[ds], (dest, f, t)
        )

    def send_kv(ds, c):
        kv_copy(ds, s, s + ds).start()
        return c

    lax.fori_loop(1, n_sp - s, send_kv, 0)

    load_copies[2].wait()
    load_copies[3].wait()
    pair = dot(normed[...], pair_w[...]).astype(bf16)
    mixed_in = (pair[:, :c0].astype(f32) * pair[:, c0:].astype(f32)).astype(bf16)
    tail[...] = mixed_in[block - 16 :, :]
    ext[pl.ds(8, block), :] = mixed_in.astype(f32)

    def halo_copy(dest):
        return rc(tail, halo, halo_send, halo_recv, (dest, f, t))

    @pl.when(s + 1 < n_sp)
    def _():
        halo_copy(s + 1).start()

    @pl.when(s == 0)
    def _():
        halo[...] = jnp.zeros_like(halo)

    load_copies[4].wait()
    load_copies[5].wait()
    rest = dot(normed[...], rest_w[...]).astype(bf16)
    for h in range(heads):
        q_buf[h] = rest[:, h * hd : (h + 1) * hd]
    post_buf[...] = rest[:, qw:]

    def absorb(si, first):
        start = pl.multiple_of(si * block, block)
        key_block = kv[pl.ds(start, block), 0:hd]
        value_block = kv[pl.ds(start, block), hd : 2 * hd]
        for h in range(heads):
            scores = (
                lax.dot_general(
                    q_buf[h], key_block, (((1,), (1,)), ((), ())), preferred_element_type=f32
                )
                * scale
            )
            gate_row = gates[pl.ds(g * heads + h, 1), pl.ds(start, block)]
            scores = scores + gate_col[h][:, 0:1] - gate_row
            if first:
                q_pos = lax.broadcasted_iota(jnp.int32, (block, block), 0)
                k_pos = lax.broadcasted_iota(jnp.int32, (block, block), 1)
                scores = jnp.where(q_pos >= k_pos, scores, masked_score)
                new_max = jnp.max(scores, axis=1, keepdims=True)
                weights = jnp.exp(scores - new_max)
                run_sum[h] = jnp.broadcast_to(jnp.sum(weights, axis=1, keepdims=True), (block, 128))
                run_max[h] = jnp.broadcast_to(new_max, (block, 128))
                acc[h] = dot(weights.astype(bf16), value_block)
            else:
                old_max = run_max[h][:, 0:1]
                new_max = jnp.maximum(old_max, jnp.max(scores, axis=1, keepdims=True))
                rescale = jnp.exp(old_max - new_max)
                weights = jnp.exp(scores - new_max)
                run_sum[h] = run_sum[h] * rescale + jnp.sum(weights, axis=1, keepdims=True)
                run_max[h] = jnp.broadcast_to(new_max, (block, 128))
                acc[h] = acc[h] * rescale + dot(weights.astype(bf16), value_block)

    absorb(s, True)

    @pl.when(s > 0)
    def _():
        halo_copy(s).wait_recv()

    ext[pl.ds(0, 8), :] = halo[...].astype(f32)[8:, :]
    tap = taps[:, pl.ds(pl.multiple_of(g * channels, channels), channels)].astype(f32)
    count = taps.shape[0]
    conv_sum = tap[0:1] * ext[pl.ds(8 - count + 1, block), :]
    for i in range(1, count):
        conv_sum = conv_sum + tap[i : i + 1] * ext[pl.ds(8 - count + 1 + i, block), :]
    mix_in[:, 0:channels] = (post_buf[...].astype(f32) * conv_sum).astype(bf16)

    def kvf_copy(ds, dt):
        i = ds * n_tp + dt
        return rc(
            kv_piece(s - ds, t), kv_piece(s - ds, t), kvf_send.at[i], kvf_recv.at[i], tp_peer(dt)
        )

    def pass_on(ds):
        kv_copy(ds, s - ds, s).wait_recv()
        for dt in range(1, n_tp):
            kvf_copy(ds, dt).start()

    @pl.when(s > 0)
    def _():
        pass_on(1)

    def earlier(ds, c):
        @pl.when(ds < s)
        def _():
            pass_on(ds + 1)

        for dt in range(1, n_tp):
            kvf_copy(ds, dt).wait_recv()
        absorb(s - ds, False)
        return c

    lax.fori_loop(1, s + 1, earlier, 0)
    for h in range(heads):
        mix_in[:, channels + h * hd : channels + (h + 1) * hd] = (
            acc[h] / run_sum[h][:, 0:1]
        ).astype(bf16)

    load_copies[6].wait()
    load_copies[7].wait()
    n_chunks = width // col_chunk

    def cols(c):
        return slice(c * col_chunk, (c + 1) * col_chunk)

    def sib_copy(c, dt):
        i = c * n_tp + dt
        return rc(
            part.at[lax.rem(t + dt, n_tp), :, cols(c)],
            sib_in.at[dt, :, cols(c)],
            sib_send.at[i],
            sib_recv.at[i],
            tp_peer(dt),
        )

    def rs_copy(c, df):
        i = c * n_fs + df
        dest = lax.rem(f + df, n_fs)
        return rc(
            pair_sum.at[pl.ds(pl.multiple_of(dest * own_rows, own_rows), own_rows), cols(c)],
            rs_in.at[df, :, cols(c)],
            rs_send.at[i],
            rs_recv.at[i],
            fs_peer(df),
        )

    for c in range(n_chunks):
        piece = dot(mix_in[...], out_w[:, cols(c)]).astype(bf16)
        for fi in range(n_fs):
            for ti in range(n_tp):
                r = (fi * n_tp + ti) * own_rows
                part[ti, fi * own_rows : (fi + 1) * own_rows, cols(c)] = piece[r : r + own_rows]
        for dt in range(1, n_tp):
            sib_copy(c, dt).start()

    for c in range(n_chunks):
        total = part[t, :, cols(c)].astype(f32)
        for dt in range(1, n_tp):
            sib_copy(c, dt).wait_recv()
            total = total + sib_in[dt, :, cols(c)].astype(f32)
        pair_sum[:, cols(c)] = total.astype(bf16)
        for df in range(1, n_fs):
            rs_copy(c, df).start()

    own = pl.ds(pl.multiple_of(f * own_rows, own_rows), own_rows)
    for c in range(n_chunks):
        total = pair_sum[own, cols(c)].astype(f32)
        for df in range(1, n_fs):
            rs_copy(c, df).wait_recv()
            total = total + rs_in[df, :, cols(c)].astype(f32)
        out[:, cols(c)] = total.astype(bf16)

    for df in range(1, n_fs):
        ag_copy(df).wait_send()
    for df in range(n_fs):
        for dt in range(1, n_tp):
            agf_copy(df, dt).wait_send()

    def kv_left(ds, c):
        kv_copy(ds, s, s + ds).wait_send()
        return c

    lax.fori_loop(1, n_sp - s, kv_left, 0)

    def kvf_left(ds, c):
        for dt in range(1, n_tp):
            kvf_copy(ds, dt).wait_send()
        return c

    lax.fori_loop(1, s + 1, kvf_left, 0)

    @pl.when(s + 1 < n_sp)
    def _():
        halo_copy(s + 1).wait_send()

    for c in range(n_chunks):
        for dt in range(1, n_tp):
            sib_copy(c, dt).wait_send()
        for df in range(1, n_fs):
            rs_copy(c, df).wait_send()


def solution(mesh):
    n_sp, n_fs, n_tp = (mesh.shape[a] for a in ("sp", "fs", "tp"))

    def shards(
        tokens,
        norm_gain,
        w_query,
        w_key,
        w_value,
        w_conv_value,
        w_conv_pre,
        w_conv_post,
        conv_taps,
        log_gate_cache,
        w_out_conv,
        w_out_attn,
    ):
        own_rows, width = tokens.shape
        block = own_rows * n_fs * n_tp
        channels = w_conv_post.shape[1]
        head_dim = w_key.shape[1]
        qw = w_query.shape[1]
        heads = qw // head_dim
        col_chunk = 512
        n_chunks = width // col_chunk
        vm = pl.BlockSpec(memory_space=pltpu.VMEM)
        hbm = pl.BlockSpec(memory_space=pl.ANY)
        V = pltpu.VMEM
        D = pltpu.SemaphoreType.DMA
        return pl.pallas_call(
            functools.partial(layer_kernel, n_sp, n_fs, n_tp, col_chunk),
            out_shape=jax.ShapeDtypeStruct((own_rows, width), bf16),
            in_specs=[vm, vm] + [hbm] * 6 + [vm, vm] + [hbm] * 2,
            out_specs=vm,
            scratch_shapes=[
                V((block, width), bf16),
                V((width, 2 * head_dim), bf16),
                V((width, 2 * channels), bf16),
                V((width, qw + channels), bf16),
                V((channels + qw, width), bf16),
                V((n_sp * block, 2 * head_dim), bf16),
                V((block + 8, channels), f32),
                V((16, channels), bf16),
                V((16, channels), bf16),
                V((block, channels), bf16),
                V((heads, block, head_dim), bf16),
                V((heads, block, 128), f32),
                V((heads, block, 128), f32),
                V((heads, block, 128), f32),
                V((heads, block, head_dim), f32),
                V((block, channels + qw), bf16),
                V((n_tp, n_fs * own_rows, width), bf16),
                V((n_tp, n_fs * own_rows, width), bf16),
                V((n_fs * own_rows, width), bf16),
                V((n_fs, own_rows, width), bf16),
                D((8,)),
                D((n_fs,)),
                D((n_fs,)),
                D((n_fs * n_tp,)),
                D((n_fs * n_tp,)),
                D((n_sp,)),
                D((n_sp,)),
                D((n_sp * n_tp,)),
                D((n_sp * n_tp,)),
                D,
                D,
                D((n_chunks * n_tp,)),
                D((n_chunks * n_tp,)),
                D((n_chunks * n_fs,)),
                D((n_chunks * n_fs,)),
            ],
            compiler_params=pltpu.CompilerParams(
                collective_id=0, has_side_effects=True, vmem_limit_bytes=60 * 1024 * 1024
            ),
        )(
            tokens,
            norm_gain.reshape(1, width),
            w_query,
            w_key,
            w_value,
            w_conv_value,
            w_conv_pre,
            w_conv_post,
            conv_taps,
            log_gate_cache,
            w_out_conv,
            w_out_attn,
        )

    placed = (
        P(("sp", "fs", "tp"), None),
        P(),
        P(None, ("fs", "tp")),
        P(None, "fs"),
        P(None, "fs"),
        P(None, ("fs", "tp")),
        P(None, ("fs", "tp")),
        P(None, ("fs", "tp")),
        P(),
        P(),
        P(("fs", "tp"), None),
        P(("fs", "tp"), None),
    )
    return jax.shard_map(
        shards, mesh=mesh, in_specs=placed, out_specs=P(("sp", "fs", "tp"), None), check_vma=False
    )
```
